32 devices in a mesh: fs: 8 (over z, y), tp: 4 (over x, core).
Axes of the slice: x: 2, y: 2, z: 4, core: 2. Of those that a mesh axis runs over, the one named last changes fastest.
Arguments:
- tokens: bfloat16 [3072, 2048], P(('fs', 'tp')), may hold values from -6 to 6
- ffn1_gain: float32 [2048], replicated, may hold values from 0.1 to 1.9
- ffn1_gate: bfloat16 [2048, 5632], P('fs', 'tp'), may hold values from -0.125 to 0.125
- ffn1_up: bfloat16 [2048, 5632], P('fs', 'tp'), may hold values from -0.125 to 0.125
- ffn1_down: bfloat16 [5632, 2048], P('tp', 'fs'), may hold values from -0.078125 to 0.078125
- mix_gain: float32 [2048], replicated, may hold values from 0.1 to 1.9
- lru_in_weight: bfloat16 [2048, 1536], P('fs', 'tp'), may hold values from -0.125 to 0.125
- lru_gate_weight: bfloat16 [2048, 1536], P('fs', 'tp'), may hold values from -0.125 to 0.125
- conv_weight: bfloat16 [4, 1536], P(None, 'tp'), may hold values from -3 to 3
- gate_a_weight: bfloat16 [24, 64, 64], P('tp'), may hold values from -0.75 to 0.75
- gate_x_weight: bfloat16 [24, 64, 64], P('tp'), may hold values from -0.75 to 0.75
- decay_param: float32 [1536], P('tp'), may hold values from 3.7 to 9
- mix_out_weight: bfloat16 [1536, 2048], P('tp', 'fs'), may hold values from -0.15625 to 0.15625
- ffn2_gain: float32 [2048], replicated, may hold values from 0.1 to 1.9
- ffn2_gate: bfloat16 [2048, 5632], P('fs', 'tp'), may hold values from -0.125 to 0.125
- ffn2_up: bfloat16 [2048, 5632], P('fs', 'tp'), may hold values from -0.125 to 0.125
- ffn2_down: bfloat16 [5632, 2048], P('tp', 'fs'), may hold values from -0.078125 to 0.078125
Outputs:
- layer_out: bfloat16 [3072, 2048], P(('fs', 'tp'))
The draws below stay inside these ranges and needn't reach their ends.
All inputs are finite; a program needn't handle non-finite values.
Results may differ from the reference program's by a relative error of at most 0.017.
Values may be sent and summed in bfloat16 or wider, within the bound.
A program may use at most 64 MiB of HBM per device.

```python
import jax
import jax.numpy as jnp
from jax import lax

D = 2048
FF = 5632
DR = 1536
LB = 64
WIDTH = 4
SEQ = 384
NB = 24
TOKENS = 3072
N_FS = 8
N_TP = 4


def draw_decay_param(key, part):
    first_key, second_key, third_key = jax.random.split(jax.random.fold_in(key, 17), 3)
    slow_share = 0.5
    slow = jax.random.bernoulli(first_key, slow_share, (DR,))
    fast_values = jax.random.uniform(second_key, (DR,), jnp.float32, 3.7, 4.9)
    slow_values = jax.random.uniform(third_key, (DR,), jnp.float32, 7.5, 9.0)
    return jnp.where(slow, slow_values, fast_values).astype(jnp.float32)


def block_scale(own_key, extent, pieces, low, largest):
    loudness = 1.0
    for dim, shards_of in pieces:
        draws = jax.random.uniform(jax.random.fold_in(jax.random.fold_in(own_key, 6), dim), (shards_of,), jnp.float32, low / len(pieces), largest / len(pieces))
        loudness = loudness * jnp.repeat(jnp.exp(draws), extent[dim] // shards_of).reshape((-1,) + (1,) * (len(extent) - 1 - dim))
    return loudness


def normal_values(key, dims, scale, limit, pieces=(), kind=jnp.bfloat16):
    level = block_scale(key, dims, pieces, -0.22, 0.18) if pieces else 1.0
    array = jax.random.normal(key, dims, jnp.float32) * scale * level
    return jnp.minimum(jnp.maximum(array, -limit), limit).astype(kind)


def setup_inputs(seed: int = 0) -> dict:
    key_list = jax.random.split(jax.random.key(seed), 18)
    return {
        "tokens": normal_values(key_list[0], (TOKENS, D), 1.0, 6.0, ((0, 32),)),
        "ffn1_gain": jnp.clip(1.0 + 0.18 * jax.random.normal(key_list[1], (D,), jnp.float32), 0.1, 1.9),
        "ffn1_gate": normal_values(key_list[2], (D, FF), D ** -0.5, 0.125, ((0, 8), (1, 4))),
        "ffn1_up": normal_values(key_list[3], (D, FF), D ** -0.5, 0.125, ((0, 8), (1, 4))),
        "ffn1_down": normal_values(key_list[4], (FF, D), FF ** -0.5, 0.078125, ((0, 4), (1, 8))),
        "mix_gain": jnp.clip(1.0 + 0.18 * jax.random.normal(key_list[5], (D,), jnp.float32), 0.1, 1.9),
        "lru_in_weight": normal_values(key_list[6], (D, DR), D ** -0.5, 0.125, ((0, 8), (1, 4))),
        "lru_gate_weight": normal_values(key_list[7], (D, DR), D ** -0.5, 0.125, ((0, 8), (1, 4))),
        "conv_weight": normal_values(key_list[8], (WIDTH, DR), WIDTH ** -0.5, 3.0, ((1, 4),)),
        "gate_a_weight": normal_values(key_list[9], (NB, LB, LB), LB ** -0.5, 0.75, ((0, 4),)),
        "gate_x_weight": normal_values(key_list[10], (NB, LB, LB), LB ** -0.5, 0.75, ((0, 4),)),
        "decay_param": draw_decay_param(jax.random.fold_in(key_list[17], 71), 0),
        "mix_out_weight": normal_values(key_list[12], (DR, D), DR ** -0.5, 0.15625, ((0, 4), (1, 8))),
        "ffn2_gain": jnp.clip(1.0 + 0.18 * jax.random.normal(key_list[13], (D,), jnp.float32), 0.1, 1.9),
        "ffn2_gate": normal_values(key_list[14], (D, FF), D ** -0.5, 0.125, ((0, 8), (1, 4))),
        "ffn2_up": normal_values(key_list[15], (D, FF), D ** -0.5, 0.125, ((0, 8), (1, 4))),
        "ffn2_down": normal_values(key_list[16], (FF, D), FF ** -0.5, 0.078125, ((0, 4), (1, 8))),
    }


EPS = 1e-06

def rms_rows(values, gain):
    wide = values.astype(jnp.float32)
    scale = lax.rsqrt(lax.optimization_barrier(jnp.mean(wide * wide, axis=-1, keepdims=True)) + EPS)
    return (wide * scale * gain.astype(jnp.float32)).astype(jnp.bfloat16)

def group_sums(hidden, weight):
    rows = hidden.shape[0]
    inner = hidden.shape[1] // N_TP
    hidden_groups = hidden.reshape(rows, N_TP, inner).transpose(1, 0, 2)
    weight_groups = weight.reshape(N_TP, inner, weight.shape[1])

    def add_group(total, pair):
        part = jnp.dot(pair[0], pair[1], preferred_element_type=jnp.float32).astype(jnp.bfloat16)
        return (total + lax.optimization_barrier(part).astype(jnp.float32), None)
    start = jnp.zeros((rows, weight.shape[1]), jnp.float32)
    total, _ = lax.scan(add_group, start, (hidden_groups, weight_groups))
    return total

def half_block(values, gain, gate_weight, up_weight, down_weight):
    normed = rms_rows(values, gain)
    gate = jnp.dot(normed, gate_weight, preferred_element_type=jnp.float32)
    upper = jnp.dot(normed, up_weight, preferred_element_type=jnp.float32)
    hidden = (jax.nn.silu(gate) * upper).astype(jnp.bfloat16)
    return group_sums(hidden, down_weight)

def combine(earlier, later):
    return (earlier[0] * later[0], later[0] * earlier[1] + later[1])

def reference(tokens, ffn1_gain, ffn1_gate, ffn1_up, ffn1_down, mix_gain, lru_in_weight, lru_gate_weight, conv_weight, gate_a_weight, gate_x_weight, decay_param, mix_out_weight, ffn2_gain, ffn2_gate, ffn2_up, ffn2_down):
    first = (tokens.astype(jnp.float32) + 0.5 * half_block(tokens, ffn1_gain, ffn1_gate, ffn1_up, ffn1_down)).astype(jnp.bfloat16)
    normed = rms_rows(first, mix_gain)
    lru_x = jnp.dot(normed, lru_in_weight, preferred_element_type=jnp.float32).astype(jnp.bfloat16)
    lru_gate = jnp.dot(normed, lru_gate_weight, preferred_element_type=jnp.float32).astype(jnp.bfloat16)
    seqs = lru_x.astype(jnp.float32).reshape(N_FS, SEQ, DR)
    padded = jnp.pad(seqs, ((0, 0), (WIDTH - 1, 0), (0, 0)))
    taps = conv_weight.astype(jnp.float32)
    conv = jnp.zeros((N_FS, SEQ, DR), jnp.float32)
    for offset in range(WIDTH):
        conv = conv + taps[offset] * padded[:, WIDTH - 1 - offset:WIDTH - 1 - offset + SEQ]
    conv_low = conv.astype(jnp.bfloat16).astype(jnp.float32)
    blocks = conv_low.reshape(N_FS, SEQ, NB, LB)
    recall = jax.nn.sigmoid(jnp.einsum('nsbi,bij->nsbj', blocks, gate_a_weight.astype(jnp.float32)).reshape(N_FS, SEQ, DR))
    admit = jax.nn.sigmoid(jnp.einsum('nsbi,bij->nsbj', blocks, gate_x_weight.astype(jnp.float32)).reshape(N_FS, SEQ, DR))
    log_keep = -8.0 * recall * jax.nn.softplus(-decay_param)
    drive = jnp.sqrt(-jnp.expm1(2.0 * log_keep)) * admit * conv_low
    _, state = lax.associative_scan(combine, (jnp.exp(log_keep), drive), axis=1)
    mixed = (state.reshape(TOKENS, DR) * jax.nn.gelu(lru_gate.astype(jnp.float32))).astype(jnp.bfloat16)
    second = (first.astype(jnp.float32) + group_sums(mixed, mix_out_weight)).astype(jnp.bfloat16)
    return (second.astype(jnp.float32) + 0.5 * half_block(second, ffn2_gain, ffn2_gate, ffn2_up, ffn2_down)).astype(jnp.bfloat16)
```

```python
import math

import jax
import jax.numpy as jnp
from jax import lax
from jax.sharding import PartitionSpec as P

EPS = 1e-06
CORES = 2
SHARE_FIRST = 4
SHARE_MIX = 2
SHARE_SECOND = 4


def rms_rows(values, gain):
    wide = values.astype(jnp.float32)
    scale = lax.rsqrt(jnp.mean(wide * wide, axis=-1, keepdims=True) + EPS)
    return (wide * scale * gain).astype(jnp.bfloat16)


def pick(stack, index):
    return lax.dynamic_index_in_dim(stack, index, 0, keepdims=False)


def share_weights(blocks, n):
    shares, high, wide = blocks.shape
    me = lax.axis_index("fs")
    chosen = [pick(blocks, (me + j) % shares) for j in range(shares)]
    whole = jnp.zeros((high, n * wide), blocks.dtype)
    for d in range(n):
        piece = chosen[d % shares]
        if d:
            piece = lax.ppermute(piece, "fs", [(i, (i + d) % n) for i in range(n)])
        whole = lax.dynamic_update_slice(whole, piece, (0, ((me - d) % n) * wide))
    return whole


def steps_of(shares, xs):
    return [(j, k) for j in range(shares) for k in range(xs)]


def route(n, t, shares, j, k):
    xs = t // CORES
    pairs = []
    for f in range(n):
        for x in range(xs):
            for c in range(CORES):
                to_f = f // shares * shares + (f % shares + j) % shares
                to_t = (x + k) % xs * CORES + c
                pairs.append((f * t + x * CORES + c, to_f * t + to_t))
    return pairs


def swap_core(values, t):
    return lax.ppermute(values, "tp", [(i, i ^ 1) for i in range(t)])


def gather_cell(rows, n, t, shares):
    got = [
        lax.ppermute(rows, ("fs", "tp"), route(n, t, shares, j, k)) if j or k else rows
        for j, k in steps_of(shares, t // CORES)
    ]
    own = jnp.concatenate(got, axis=0)
    return own, swap_core(own, t)


def scatter_cell(own, other, local, n, t, shares):
    xs = t // CORES
    both = own + swap_core(other.astype(jnp.bfloat16), t).astype(jnp.float32)
    low = both.astype(jnp.bfloat16)
    total = both[:local]
    for s, (j, k) in enumerate(steps_of(shares, xs)):
        if s:
            back = [(b, a) for a, b in route(n, t, shares, j, k)]
            total = total + lax.ppermute(
                low[s * local : (s + 1) * local], ("fs", "tp"), back
            ).astype(jnp.float32)
    return total


def dot_nt(a, b):
    return lax.dot_general(a, b, (((1,), (1,)), ((), ())), preferred_element_type=jnp.float32)


def in_pair(first, second, shares, n):
    stack = jnp.concatenate(
        [w.T.reshape(shares, -1, w.shape[0]) for w in (first, second)], axis=1
    )
    return share_weights(stack, n)


def out_share(weight, shares, n):
    return share_weights(weight.reshape(shares, -1, weight.shape[1]), n)


def half_block(normed, pair, down, n, t, shares):
    half = pair.shape[0] // 2

    def terms(rows):
        both = dot_nt(rows, pair)
        hidden = (jax.nn.silu(both[:, :half]) * both[:, half:]).astype(jnp.bfloat16)
        return jnp.dot(hidden, down, preferred_element_type=jnp.float32)

    own, other = gather_cell(normed, n, t, shares)
    other_terms = terms(other)
    return scatter_cell(terms(own), other_terms, normed.shape[0], n, t, shares)


def combine(earlier, later):
    return (earlier[0] * later[0], later[0] * earlier[1] + later[1])


def mixer(normed, pair, out, conv_weight, gate_a_weight, gate_x_weight, decay_param, n, t, shares):
    local = normed.shape[0]
    xs = t // CORES
    place = lax.axis_index("fs") % shares
    tp = lax.axis_index("tp")
    x, core = tp // CORES, tp % CORES
    steps = steps_of(shares, xs)
    own, other = gather_cell(normed, n, t, shares)
    low = jnp.concatenate([dot_nt(own, pair), dot_nt(other, pair)], axis=0).astype(jnp.bfloat16)
    width = low.shape[1]
    low = low.reshape(2 * len(steps), local, width)
    ordered = []
    for s in range(shares):
        for a in range(xs):
            at = ((place - s) % shares) * xs + (x - a) % xs
            for c in range(CORES):
                ordered.append(pick(low, at + jnp.where(core == c, 0, len(steps))))
    channels = width // 2
    both = jnp.concatenate(ordered, axis=0).reshape(shares, t * local, width).astype(jnp.float32)
    lru_low, gate_low = both[..., :channels], both[..., channels:]
    blocks_here = gate_a_weight.shape[0] // shares
    size = gate_a_weight.shape[1]
    gate_a = lax.dynamic_slice_in_dim(gate_a_weight, place * blocks_here, blocks_here, 0)
    gate_x = lax.dynamic_slice_in_dim(gate_x_weight, place * blocks_here, blocks_here, 0)
    taps = lax.dynamic_slice_in_dim(conv_weight, place * channels, channels, 1).astype(jnp.float32)
    decay = lax.dynamic_slice_in_dim(decay_param, place * channels, channels, 0)
    length = t * local
    count = taps.shape[0]
    padded = jnp.pad(lru_low, ((0, 0), (count - 1, 0), (0, 0)))
    conv = jnp.zeros_like(lru_low)
    for offset in range(count):
        conv = conv + taps[offset] * padded[:, count - 1 - offset : count - 1 - offset + length]
    conv_low = conv.astype(jnp.bfloat16)
    eye = jnp.eye(blocks_here, dtype=jnp.bfloat16)
    flat = conv_low.reshape(shares * length, channels)

    def gate(weight):
        dense = (eye[:, None, :, None] * weight[:, :, None, :]).reshape(channels, channels)
        return jax.nn.sigmoid(
            jnp.dot(flat, dense, preferred_element_type=jnp.float32)
        ).reshape(shares, length, channels)

    recall, admit = gate(gate_a), gate(gate_x)
    log_keep = -8.0 * recall * jax.nn.softplus(-decay)
    drive = jnp.sqrt(-jnp.expm1(2.0 * log_keep)) * admit * conv_low.astype(jnp.float32)
    _, state = lax.associative_scan(combine, (jnp.exp(log_keep), drive), axis=1)
    mixed = (state * jax.nn.gelu(gate_low)).astype(jnp.bfloat16)
    mixed = mixed.reshape(shares * t, local, channels)
    sides = []
    for side in (core, 1 - core):
        rows = [
            pick(mixed, ((place - j) % shares) * t + ((x - k) % xs) * CORES + side)
            for j, k in steps
        ]
        sides.append(
            jnp.dot(jnp.concatenate(rows, axis=0), out, preferred_element_type=jnp.float32)
        )
    return scatter_cell(sides[0], sides[1], local, n, t, shares)


def body(
    n,
    t,
    tokens,
    ffn1_gain,
    ffn1_gate,
    ffn1_up,
    ffn1_down,
    mix_gain,
    lru_in_weight,
    lru_gate_weight,
    conv_weight,
    gate_a_weight,
    gate_x_weight,
    decay_param,
    mix_out_weight,
    ffn2_gain,
    ffn2_gate,
    ffn2_up,
    ffn2_down,
):
    share_mix = math.gcd(SHARE_MIX, gate_a_weight.shape[0], n)
    pair1 = in_pair(ffn1_gate, ffn1_up, SHARE_FIRST, n)
    down1 = out_share(ffn1_down, SHARE_FIRST, n)
    pair_mix = in_pair(lru_in_weight, lru_gate_weight, share_mix, n)
    out_mix = out_share(mix_out_weight, share_mix, n)
    pair2 = in_pair(ffn2_gate, ffn2_up, SHARE_SECOND, n)
    down2 = out_share(ffn2_down, SHARE_SECOND, n)
    sums = half_block(rms_rows(tokens, ffn1_gain), pair1, down1, n, t, SHARE_FIRST)
    first = (tokens.astype(jnp.float32) + 0.5 * sums).astype(jnp.bfloat16)
    sums = mixer(
        rms_rows(first, mix_gain),
        pair_mix,
        out_mix,
        conv_weight,
        gate_a_weight,
        gate_x_weight,
        decay_param,
        n,
        t,
        share_mix,
    )
    second = (first.astype(jnp.float32) + sums).astype(jnp.bfloat16)
    sums = half_block(rms_rows(second, ffn2_gain), pair2, down2, n, t, SHARE_SECOND)
    return (second.astype(jnp.float32) + 0.5 * sums).astype(jnp.bfloat16)


def solution(mesh):
    n, t = mesh.shape["fs"], mesh.shape["tp"]
    in_specs = (
        P(("fs", "tp"), None),
        P(),
        P("fs", "tp"),
        P("fs", "tp"),
        P("tp", "fs"),
        P(),
        P("fs", "tp"),
        P("fs", "tp"),
        P(None, "tp"),
        P("tp", None, None),
        P("tp", None, None),
        P("tp"),
        P("tp", "fs"),
        P(),
        P("fs", "tp"),
        P("fs", "tp"),
        P("tp", "fs"),
    )
    out_specs = P(("fs", "tp"), None)

    def run(*args):
        return body(n, t, *args)

    return jax.shard_map(run, mesh=mesh, in_specs=in_specs, out_specs=out_specs, check_vma=False)
```

```python
import math

import jax
import jax.numpy as jnp
from jax import lax
from jax.experimental import pallas as pl
from jax.sharding import PartitionSpec as P

EPS = 1e-06
CORES = 2
SHARE_FIRST = 4
SHARE_MIX = 2
SHARE_SECOND = 4


def rms_rows(values, gain):
    wide = values.astype(jnp.float32)
    scale = lax.rsqrt(jnp.mean(wide * wide, axis=-1, keepdims=True) + EPS)
    return (wide * scale * gain).astype(jnp.bfloat16)


def pick(stack, index):
    return lax.dynamic_index_in_dim(stack, index, 0, keepdims=False)


def share_weights(blocks, n):
    shares, high, wide = blocks.shape
    me = lax.axis_index("fs")
    chosen = [pick(blocks, (me + j) % shares) for j in range(shares)]
    whole = jnp.zeros((high, n * wide), blocks.dtype)
    for d in range(n):
        piece = chosen[d % shares]
        if d:
            piece = lax.ppermute(piece, "fs", [(i, (i + d) % n) for i in range(n)])
        whole = lax.dynamic_update_slice(whole, piece, (0, ((me - d) % n) * wide))
    return whole


def steps_of(shares, xs):
    return [(j, k) for j in range(shares) for k in range(xs)]


def route(n, t, shares, j, k):
    xs = t // CORES
    pairs = []
    for f in range(n):
        for x in range(xs):
            for c in range(CORES):
                to_f = f // shares * shares + (f % shares + j) % shares
                to_t = (x + k) % xs * CORES + c
                pairs.append((f * t + x * CORES + c, to_f * t + to_t))
    return pairs


def swap_core(values, t):
    return lax.ppermute(values, "tp", [(i, i ^ 1) for i in range(t)])


def send(values, pairs):
    return lax.ppermute(values, ("fs", "tp"), pairs)


def gather_cell(rows, n, t, shares):
    got = [
        send(rows, route(n, t, shares, j, k)) if j or k else rows
        for j, k in steps_of(shares, t // CORES)
    ]
    own = jnp.concatenate(got, axis=0)
    return own, swap_core(own, t)


def scatter_cell(own, other, local, n, t, shares):
    xs = t // CORES
    both = own + swap_core(other.astype(jnp.bfloat16), t).astype(jnp.float32)
    low = both.astype(jnp.bfloat16)
    total = both[:local]
    for s, (j, k) in enumerate(steps_of(shares, xs)):
        if s:
            back = [(b, a) for a, b in route(n, t, shares, j, k)]
            part = send(low[s * local : (s + 1) * local], back)
            total = total + part.astype(jnp.float32)
    return total


def dot_nt(a, b):
    return lax.dot_general(a, b, (((1,), (1,)), ((), ())), preferred_element_type=jnp.float32)


def in_pair(first, second, shares, n):
    stack = jnp.concatenate(
        [w.T.reshape(shares, -1, w.shape[0]) for w in (first, second)], axis=1
    )
    return share_weights(stack, n)


def out_share(weight, shares, n):
    return share_weights(weight.reshape(shares, -1, weight.shape[1]), n)


def half_block(normed, pair, down, n, t, shares):
    half = pair.shape[0] // 2

    def terms(rows):
        both = dot_nt(rows, pair)
        hidden = (jax.nn.silu(both[:, :half]) * both[:, half:]).astype(jnp.bfloat16)
        return jnp.dot(hidden, down, preferred_element_type=jnp.float32)

    own, other = gather_cell(normed, n, t, shares)
    other_terms = terms(other)
    return scatter_cell(terms(own), other_terms, normed.shape[0], n, t, shares)


def scan_kernel(keep_ref, drive_ref, out_ref):
    keep, state = keep_ref[0], drive_ref[0]
    length = keep.shape[0]
    step = 1
    while step < length:
        ones = jnp.ones((step, keep.shape[1]), jnp.float32)
        zeros = jnp.zeros((step, keep.shape[1]), jnp.float32)
        state = state + keep * jnp.concatenate([zeros, state[: length - step]], axis=0)
        keep = keep * jnp.concatenate([ones, keep[: length - step]], axis=0)
        step *= 2
    out_ref[0] = state


def scan_rows(keep, drive):
    seqs, length, channels = keep.shape
    spec = pl.BlockSpec((1, length, channels), lambda i: (i, 0, 0))
    return pl.pallas_call(
        scan_kernel,
        grid=(seqs,),
        in_specs=[spec, spec],
        out_specs=spec,
        out_shape=jax.ShapeDtypeStruct(keep.shape, jnp.float32),
        cost_estimate=pl.CostEstimate(
            flops=30 * keep.size, bytes_accessed=12 * keep.size, transcendentals=0
        ),
    )(keep, drive)


def mixer(normed, pair, out, conv_weight, gate_a_weight, gate_x_weight, decay_param, n, t, shares):
    local = normed.shape[0]
    xs = t // CORES
    place = lax.axis_index("fs") % shares
    tp = lax.axis_index("tp")
    x, core = tp // CORES, tp % CORES
    steps = steps_of(shares, xs)
    own, other = gather_cell(normed, n, t, shares)
    low = jnp.concatenate([dot_nt(own, pair), dot_nt(other, pair)], axis=0).astype(jnp.bfloat16)
    width = low.shape[1]
    low = low.reshape(2 * len(steps), local, width)
    ordered = []
    for s in range(shares):
        for a in range(xs):
            at = ((place - s) % shares) * xs + (x - a) % xs
            for c in range(CORES):
                ordered.append(pick(low, at + jnp.where(core == c, 0, len(steps))))
    channels = width // 2
    both = jnp.concatenate(ordered, axis=0).reshape(shares, t * local, width).astype(jnp.float32)
    lru_low, gate_low = both[..., :channels], both[..., channels:]
    blocks_here = gate_a_weight.shape[0] // shares
    gate_a = lax.dynamic_slice_in_dim(gate_a_weight, place * blocks_here, blocks_here, 0)
    gate_x = lax.dynamic_slice_in_dim(gate_x_weight, place * blocks_here, blocks_here, 0)
    taps = lax.dynamic_slice_in_dim(conv_weight, place * channels, channels, 1).astype(jnp.float32)
    decay = lax.dynamic_slice_in_dim(decay_param, place * channels, channels, 0)
    length = t * local
    count = taps.shape[0]
    padded = jnp.pad(lru_low, ((0, 0), (count - 1, 0), (0, 0)))
    conv = jnp.zeros_like(lru_low)
    for offset in range(count):
        conv = conv + taps[offset] * padded[:, count - 1 - offset : count - 1 - offset + length]
    conv_low = conv.astype(jnp.bfloat16)
    eye = jnp.eye(blocks_here, dtype=jnp.bfloat16)
    flat = conv_low.reshape(shares * length, channels)

    def gate(weight):
        dense = (eye[:, None, :, None] * weight[:, :, None, :]).reshape(channels, channels)
        return jax.nn.sigmoid(
            jnp.dot(flat, dense, preferred_element_type=jnp.float32)
        ).reshape(shares, length, channels)

    recall, admit = gate(gate_a), gate(gate_x)
    log_keep = -8.0 * recall * jax.nn.softplus(-decay)
    drive = jnp.sqrt(-jnp.expm1(2.0 * log_keep)) * admit * conv_low.astype(jnp.float32)
    state = scan_rows(jnp.exp(log_keep), drive)
    mixed = (state * jax.nn.gelu(gate_low)).astype(jnp.bfloat16)
    mixed = mixed.reshape(shares * t, local, channels)
    sides = []
    for side in (core, 1 - core):
        rows = [
            pick(mixed, ((place - j) % shares) * t + ((x - k) % xs) * CORES + side)
            for j, k in steps
        ]
        sides.append(
            jnp.dot(jnp.concatenate(rows, axis=0), out, preferred_element_type=jnp.float32)
        )
    return scatter_cell(sides[0], sides[1], local, n, t, shares)


def body(
    n,
    t,
    tokens,
    ffn1_gain,
    ffn1_gate,
    ffn1_up,
    ffn1_down,
    mix_gain,
    lru_in_weight,
    lru_gate_weight,
    conv_weight,
    gate_a_weight,
    gate_x_weight,
    decay_param,
    mix_out_weight,
    ffn2_gain,
    ffn2_gate,
    ffn2_up,
    ffn2_down,
):
    share_mix = math.gcd(SHARE_MIX, gate_a_weight.shape[0], n)
    pair1 = in_pair(ffn1_gate, ffn1_up, SHARE_FIRST, n)
    down1 = out_share(ffn1_down, SHARE_FIRST, n)
    pair_mix = in_pair(lru_in_weight, lru_gate_weight, share_mix, n)
    out_mix = out_share(mix_out_weight, share_mix, n)
    pair2 = in_pair(ffn2_gate, ffn2_up, SHARE_SECOND, n)
    down2 = out_share(ffn2_down, SHARE_SECOND, n)
    sums = half_block(rms_rows(tokens, ffn1_gain), pair1, down1, n, t, SHARE_FIRST)
    first = (tokens.astype(jnp.float32) + 0.5 * sums).astype(jnp.bfloat16)
    sums = mixer(
        rms_rows(first, mix_gain),
        pair_mix,
        out_mix,
        conv_weight,
        gate_a_weight,
        gate_x_weight,
        decay_param,
        n,
        t,
        share_mix,
    )
    second = (first.astype(jnp.float32) + sums).astype(jnp.bfloat16)
    sums = half_block(rms_rows(second, ffn2_gain), pair2, down2, n, t, SHARE_SECOND)
    return (second.astype(jnp.float32) + 0.5 * sums).astype(jnp.bfloat16)


def solution(mesh):
    n, t = mesh.shape["fs"], mesh.shape["tp"]
    in_specs = (
        P(("fs", "tp"), None),
        P(),
        P("fs", "tp"),
        P("fs", "tp"),
        P("tp", "fs"),
        P(),
        P("fs", "tp"),
        P("fs", "tp"),
        P(None, "tp"),
        P("tp", None, None),
        P("tp", None, None),
        P("tp"),
        P("tp", "fs"),
        P(),
        P("fs", "tp"),
        P("fs", "tp"),
        P("tp", "fs"),
    )
    out_specs = P(("fs", "tp"), None)

    def run(*args):
        return body(n, t, *args)

    return jax.shard_map(run, mesh=mesh, in_specs=in_specs, out_specs=out_specs, check_vma=False)
```

```python
import math

import jax
import jax.numpy as jnp
from jax import lax
from jax.experimental import pallas as pl
from jax.sharding import PartitionSpec as P

EPS = 1e-06
CORES = 2
SHARE_FIRST = 4
SHARE_MIX = 2
SHARE_SECOND = 4


def rms_rows(values, gain):
    wide = values.astype(jnp.float32)
    scale = lax.rsqrt(jnp.mean(wide * wide, axis=-1, keepdims=True) + EPS)
    return (wide * scale * gain).astype(jnp.bfloat16)


def pick(stack, index):
    return lax.dynamic_index_in_dim(stack, index, 0, keepdims=False)


def send_shares(blocks, n):
    shares = blocks.shape[0]
    me = lax.axis_index("fs")
    pieces = []
    for d in range(n):
        piece = pick(blocks, (me + d) % shares)
        if d:
            piece = lax.ppermute(piece, "fs", [(i, (i + d) % n) for i in range(n)])
        pieces.append(piece)
    return pieces


def assemble(pieces, tie=None):
    n = len(pieces)
    high, wide = pieces[0].shape
    me = lax.axis_index("fs")
    whole = jnp.zeros((high, n * wide), pieces[0].dtype)
    for d, piece in enumerate(pieces):
        if d and tie is not None:
            piece, _ = lax.optimization_barrier((piece, tie))
        whole = lax.dynamic_update_slice(whole, piece, (0, ((me - d) % n) * wide))
    return whole


def steps_of(shares, xs):
    return [(j, k) for j in range(shares) for k in range(xs)]


def route(n, t, shares, j, k):
    xs = t // CORES
    pairs = []
    for f in range(n):
        for x in range(xs):
            for c in range(CORES):
                to_f = f // shares * shares + (f % shares + j) % shares
                to_t = (x + k) % xs * CORES + c
                pairs.append((f * t + x * CORES + c, to_f * t + to_t))
    return pairs


def swap_core(values, t):
    return lax.ppermute(values, "tp", [(i, i ^ 1) for i in range(t)])


def send(values, pairs):
    return lax.ppermute(values, ("fs", "tp"), pairs)


def gather_own(rows, n, t, shares):
    got = [
        send(rows, route(n, t, shares, j, k)) if j or k else rows
        for j, k in steps_of(shares, t // CORES)
    ]
    return jnp.concatenate(got, axis=0), got[1]


def scatter_cell(own, other, local, n, t, shares):
    xs = t // CORES
    both = own + swap_core(other.astype(jnp.bfloat16), t).astype(jnp.float32)
    low = both.astype(jnp.bfloat16)
    total, early = both[:local], None
    for s, (j, k) in enumerate(steps_of(shares, xs)):
        if s:
            back = [(b, a) for a, b in route(n, t, shares, j, k)]
            part = send(low[s * local : (s + 1) * local], back)
            early = part if early is None else early
            total = total + part.astype(jnp.float32)
    return total, early


def dot_nt(a, b):
    return lax.dot_general(a, b, (((1,), (1,)), ((), ())), preferred_element_type=jnp.float32)


def gather_shares(first, second, out, shares, n):
    stack = jnp.concatenate(
        [w.reshape(shares, -1, w.shape[1]) for w in (first.T, second.T, out)], axis=1
    )
    return send_shares(stack, n)


def half_block(normed, pieces, n, t, shares, late):
    own, early = gather_own(normed, n, t, shares)
    other = swap_core(own, t)
    weights = assemble(pieces, early if late else None)
    part = weights.shape[0] // 3
    own, weights = lax.optimization_barrier((own, weights))

    def terms(rows):
        both = dot_nt(rows, weights[: 2 * part])
        hidden = (jax.nn.silu(both[:, :part]) * both[:, part:]).astype(jnp.bfloat16)
        return jnp.dot(hidden, weights[2 * part :], preferred_element_type=jnp.float32)

    other_terms = terms(other)
    return scatter_cell(terms(own), other_terms, normed.shape[0], n, t, shares)


def scan_kernel(keep_ref, drive_ref, out_ref):
    keep, state = keep_ref[0], drive_ref[0]
    length = keep.shape[0]
    step = 1
    while step < length:
        ones = jnp.ones((step, keep.shape[1]), jnp.float32)
        zeros = jnp.zeros((step, keep.shape[1]), jnp.float32)
        state = state + keep * jnp.concatenate([zeros, state[: length - step]], axis=0)
        keep = keep * jnp.concatenate([ones, keep[: length - step]], axis=0)
        step *= 2
    out_ref[0] = state


def scan_rows(keep, drive):
    seqs, length, channels = keep.shape
    spec = pl.BlockSpec((1, length, channels), lambda i: (i, 0, 0))
    return pl.pallas_call(
        scan_kernel,
        grid=(seqs,),
        in_specs=[spec, spec],
        out_specs=spec,
        out_shape=jax.ShapeDtypeStruct(keep.shape, jnp.float32),
        cost_estimate=pl.CostEstimate(
            flops=30 * keep.size, bytes_accessed=12 * keep.size, transcendentals=0
        ),
    )(keep, drive)


def mixer(normed, weights, conv_weight, gate_a_weight, gate_x_weight, decay_param, n, t, shares):
    local = normed.shape[0]
    xs = t // CORES
    place = lax.axis_index("fs") % shares
    tp = lax.axis_index("tp")
    x, core = tp // CORES, tp % CORES
    steps = steps_of(shares, xs)
    part = weights.shape[0] // 3
    pair, out = weights[: 2 * part], weights[2 * part :]
    own, _ = gather_own(normed, n, t, shares)
    other = swap_core(own, t)
    low = jnp.concatenate([dot_nt(own, pair), dot_nt(other, pair)], axis=0).astype(jnp.bfloat16)
    width = low.shape[1]
    low = low.reshape(2 * len(steps), local, width)
    ordered = []
    for s in range(shares):
        for a in range(xs):
            at = ((place - s) % shares) * xs + (x - a) % xs
            for c in range(CORES):
                ordered.append(pick(low, at + jnp.where(core == c, 0, len(steps))))
    channels = width // 2
    both = jnp.concatenate(ordered, axis=0).reshape(shares, t * local, width).astype(jnp.float32)
    lru_low, gate_low = both[..., :channels], both[..., channels:]
    blocks_here = gate_a_weight.shape[0] // shares
    gate_a = lax.dynamic_slice_in_dim(gate_a_weight, place * blocks_here, blocks_here, 0)
    gate_x = lax.dynamic_slice_in_dim(gate_x_weight, place * blocks_here, blocks_here, 0)
    taps = lax.dynamic_slice_in_dim(conv_weight, place * channels, channels, 1).astype(jnp.float32)
    decay = lax.dynamic_slice_in_dim(decay_param, place * channels, channels, 0)
    length = t * local
    count = taps.shape[0]
    padded = jnp.pad(lru_low, ((0, 0), (count - 1, 0), (0, 0)))
    conv = jnp.zeros_like(lru_low)
    for offset in range(count):
        conv = conv + taps[offset] * padded[:, count - 1 - offset : count - 1 - offset + length]
    conv_low = conv.astype(jnp.bfloat16)
    eye = jnp.eye(blocks_here, dtype=jnp.bfloat16)
    flat = conv_low.reshape(shares * length, channels)

    def gate(weight):
        dense = (eye[:, None, :, None] * weight[:, :, None, :]).reshape(channels, channels)
        return jax.nn.sigmoid(
            jnp.dot(flat, dense, preferred_element_type=jnp.float32)
        ).reshape(shares, length, channels)

    recall, admit = gate(gate_a), gate(gate_x)
    log_keep = -8.0 * recall * jax.nn.softplus(-decay)
    drive = jnp.sqrt(-jnp.expm1(2.0 * log_keep)) * admit * conv_low.astype(jnp.float32)
    state = scan_rows(jnp.exp(log_keep), drive)
    mixed = (state * jax.nn.gelu(gate_low)).astype(jnp.bfloat16)
    mixed = mixed.reshape(shares * t, local, channels)
    sides = []
    for side in (core, 1 - core):
        rows = [
            pick(mixed, ((place - j) % shares) * t + ((x - k) % xs) * CORES + side)
            for j, k in steps
        ]
        sides.append(
            jnp.dot(jnp.concatenate(rows, axis=0), out, preferred_element_type=jnp.float32)
        )
    return scatter_cell(sides[0], sides[1], local, n, t, shares)


def body(
    n,
    t,
    tokens,
    ffn1_gain,
    ffn1_gate,
    ffn1_up,
    ffn1_down,
    mix_gain,
    lru_in_weight,
    lru_gate_weight,
    conv_weight,
    gate_a_weight,
    gate_x_weight,
    decay_param,
    mix_out_weight,
    ffn2_gain,
    ffn2_gate,
    ffn2_up,
    ffn2_down,
):
    share_mix = math.gcd(SHARE_MIX, gate_a_weight.shape[0], n)
    pieces1 = gather_shares(ffn1_gate, ffn1_up, ffn1_down, SHARE_FIRST, n)
    pieces_mix = gather_shares(lru_in_weight, lru_gate_weight, mix_out_weight, share_mix, n)
    pieces2 = gather_shares(ffn2_gate, ffn2_up, ffn2_down, SHARE_SECOND, n)
    sums, early = half_block(rms_rows(tokens, ffn1_gain), pieces1, n, t, SHARE_FIRST, False)
    sums, weights_mix = lax.optimization_barrier((sums, assemble(pieces_mix, early)))
    first = (tokens.astype(jnp.float32) + 0.5 * sums).astype(jnp.bfloat16)
    sums, _ = mixer(
        rms_rows(first, mix_gain),
        weights_mix,
        conv_weight,
        gate_a_weight,
        gate_x_weight,
        decay_param,
        n,
        t,
        share_mix,
    )
    second = (first.astype(jnp.float32) + sums).astype(jnp.bfloat16)
    sums, _ = half_block(rms_rows(second, ffn2_gain), pieces2, n, t, SHARE_SECOND, True)
    return (second.astype(jnp.float32) + 0.5 * sums).astype(jnp.bfloat16)


def solution(mesh):
    n, t = mesh.shape["fs"], mesh.shape["tp"]
    in_specs = (
        P(("fs", "tp"), None),
        P(),
        P("fs", "tp"),
        P("fs", "tp"),
        P("tp", "fs"),
        P(),
        P("fs", "tp"),
        P("fs", "tp"),
        P(None, "tp"),
        P("tp", None, None),
        P("tp", None, None),
        P("tp"),
        P("tp", "fs"),
        P(),
        P("fs", "tp"),
        P("fs", "tp"),
        P("tp", "fs"),
    )
    out_specs = P(("fs", "tp"), None)

    def run(*args):
        return body(n, t, *args)

    return jax.shard_map(run, mesh=mesh, in_specs=in_specs, out_specs=out_specs, check_vma=False)
```
